32 devices in a mesh: rep: 8 (over z, y), fs: 2 (over core), tp: 2 (over x).
Axes of the slice: x: 2, y: 2, z: 4, core: 2. Of those that a mesh axis runs over, the one named last changes fastest.
Arguments:
- inputs: bfloat16 [2048, 2048], P(('rep', 'fs'), 'tp'), may hold values from -6 to 6
- cotangent: bfloat16 [2048, 2048], P(('rep', 'fs'), 'tp'), may hold values from -6 to 6
- w_up: bfloat16 [2048, 4096], P('fs', 'tp'), may hold values from -0.125 to 0.125
- w_down: bfloat16 [4096, 2048], P('tp', 'fs'), may hold values from -0.09375 to 0.09375
Outputs:
- grad_inputs: bfloat16 [2048, 2048], P(('rep', 'fs'), 'tp')
- grad_up: float32 [2048, 4096], P('fs', 'tp')
- grad_down: float32 [4096, 2048], P('tp', 'fs')
The draws below stay inside these ranges and needn't reach their ends.
All inputs are finite; a program needn't handle non-finite values.
Results may differ from the reference program's by a relative error of at most 0.011.
Values may be sent and summed in bfloat16 or wider, within the bound.
A program may use at most 128 MiB of HBM per device.

```python
import jax
import jax.numpy as jnp
from jax import lax

D = 2048
FF = 4096
TOKENS = 2048
N_TP = 2


def raised(entries, key, source, target, parts, factor):
    owner, partner = [(jnp.arange(entries.shape[axis_at]) // (entries.shape[axis_at] // parts)).reshape([-1 if axis == axis_at else 1 for axis in range(entries.ndim)]) for axis_at in (source, target)]
    chosen = jax.random.permutation(key, parts)[partner]
    strong = (owner == chosen) | (owner == (partner + parts // 2) % parts)
    return jnp.where(strong, factor * entries, entries)


def levels(own_key, shape, pieces, low, largest):
    def one(position, shards_of):
        heights = jax.random.uniform(jax.random.fold_in(jax.random.fold_in(own_key, 6), position), (shards_of,), jnp.float32, low / len(pieces), largest / len(pieces))
        return jnp.repeat(jnp.exp(heights), shape[position] // shards_of).reshape((-1,) + (1,) * (len(shape) - position - 1))

    loudness = one(*pieces[0])
    for cut in pieces[1:]:
        loudness = loudness * one(*cut)
    return loudness


def normal_values(rng, shape, width, most, split=(), dtype=jnp.bfloat16):
    entries = jax.random.normal(rng, shape, jnp.float32) * width
    if len(split) > 0:
        entries = levels(rng, shape, split, -0.22, 0.18) * entries
    return jnp.clip(entries, min=-most, max=most).astype(dtype)


def bell_draw_with(rng, extent, deviation, limit, cuts, heavy, dtype=jnp.bfloat16):
    values = deviation * jax.random.normal(rng, extent, jnp.float32)
    if cuts:
        values = values * levels(rng, extent, cuts, -0.22, 0.18)
    return jnp.clip(raised(values, jax.random.fold_in(rng, 3), *heavy), -limit, limit).astype(dtype)


def setup_inputs(seed: int = 0) -> dict:
    arg_keys = jax.random.split(jax.random.key(seed), 5)
    return {
        "inputs": bell_draw_with(arg_keys[0], (TOKENS, D), 1.0, 6.0, ((0, 16), (1, 2)), (0, 1, 16, 2.0)),
        "cotangent": bell_draw_with(arg_keys[1], (TOKENS, D), 1.0, 6.0, ((0, 16), (1, 2)), (0, 1, 16, 2.0)),
        "w_up": normal_values(arg_keys[2], (D, FF), D ** -0.5, 0.125, ((0, 2), (1, 2))),
        "w_down": normal_values(arg_keys[3], (FF, D), FF ** -0.5, 0.09375, ((0, 2), (1, 2))),
    }


def reference(inputs, cotangent, w_up, w_down):
    preact = jnp.dot(inputs, w_up, preferred_element_type=jnp.float32)
    relu_pre = jnp.maximum(preact, 0.0)
    squared = (relu_pre * relu_pre).astype(jnp.bfloat16)
    act_grad = jnp.dot(cotangent, w_down.T, preferred_element_type=jnp.float32)
    pre_grad = (2.0 * relu_pre * act_grad).astype(jnp.bfloat16)
    grad_up = jnp.dot(inputs.T, pre_grad, preferred_element_type=jnp.float32)
    grad_down = jnp.dot(squared.T, cotangent, preferred_element_type=jnp.float32)
    group = w_up.shape[1] // N_TP
    total = jnp.zeros(inputs.shape, jnp.float32)
    for index in range(N_TP):
        partial_value = jnp.dot(pre_grad[:, index * group:(index + 1) * group],
                          w_up[:, index * group:(index + 1) * group].T,
                          preferred_element_type=jnp.float32).astype(jnp.bfloat16)
        partial_value = lax.optimization_barrier(partial_value)
        total = total + partial_value.astype(jnp.float32)
    return total.astype(jnp.bfloat16), grad_up, grad_down
```

```python
import functools

import jax
import jax.numpy as jnp
from jax import lax
from jax.experimental import pallas as pl
from jax.experimental.pallas import tpu as pltpu
from jax.sharding import PartitionSpec as P

MESH = pl.DeviceIdType.MESH
X, Y, UP, DOWN = range(4)
PAIR = 2


def contract_rows(left, right):
    return lax.dot_general(
        left, right, (((0,), (0,)), ((), ())), preferred_element_type=jnp.float32
    )


def contract_cols(left, right):
    return lax.dot_general(
        left, right, (((1,), (1,)), ((), ())), preferred_element_type=jnp.float32
    )


def gather_kernel(reps, x_ref, c_ref, up_ref, down_ref, gx, gc, up_other, down_other,
                  send_sem, recv_sem, swap_sem, own_sem):
    rep, fs, tp = lax.axis_index("rep"), lax.axis_index("fs"), lax.axis_index("tp")
    z, y = rep // PAIR, rep % PAIR
    depth = reps // PAIR
    half = x_ref.shape[0] // 2
    target = {
        X: {"tp": 1 - tp},
        Y: {"rep": z * PAIR + (1 - y)},
        UP: {"rep": jnp.minimum(z + 1, depth - 1) * PAIR + y},
        DOWN: {"rep": jnp.maximum(z - 1, 0) * PAIR + y},
    }
    sibling = {"fs": 1 - fs}

    def when(condition, body):
        if condition is True:
            body()
        else:
            pl.when(condition)(body)

    barrier = pltpu.get_barrier_semaphore()

    def greet(device):
        pl.semaphore_signal(barrier, inc=1, device_id=device, device_id_type=MESH)

    greet(target[X])
    greet(target[Y])
    greet(sibling)
    when(z < depth - 1, lambda: greet(target[UP]))
    when(z > 0, lambda: greet(target[DOWN]))
    pl.semaphore_wait(barrier, 3 + (z < depth - 1).astype(jnp.int32) + (z > 0).astype(jnp.int32))

    def copy(way, sub, at, own=False):
        at_z, at_y, at_t = at
        array, part = sub
        rows = pl.ds(part * half, half)
        source = at_z * PAIR + at_y
        slot = (at_t + fs) % 2
        there = (gx, gc)[array].at[slot, source, rows]
        here = (x_ref, c_ref)[array].at[rows] if own else there
        index, piece = array * 2 + part, source * 2 + at_t
        return pltpu.make_async_remote_copy(
            src_ref=here, dst_ref=there,
            send_sem=send_sem.at[way, index, piece],
            recv_sem=recv_sem.at[index, piece],
            device_id=target[way], device_id_type=MESH,
        )

    started = []

    def start(way, sub, at, condition=True, own=False):
        when(condition, lambda: copy(way, sub, at, own).start())
        started.append((way, sub, at, condition, own))

    def arrive(sub, at, condition=True):
        when(condition, lambda: copy(X, sub, at).wait_recv())

    subs = [(array, part) for part in range(2) for array in range(2)]
    first = [(array, 0) for array in range(2)]
    second = [(array, 1) for array in range(2)]

    swaps = [
        pltpu.make_async_remote_copy(
            src_ref=mine, dst_ref=theirs, send_sem=swap_sem.at[0, index], recv_sem=swap_sem.at[1, index],
            device_id=sibling, device_id_type=MESH,
        )
        for index, (mine, theirs) in enumerate(((up_ref, up_other), (down_ref, down_other)))
    ]

    here = (z, y, tp)
    for sub in subs:
        start(UP, sub, here, z < depth - 1, own=True)
        start(DOWN, sub, here, z > 0, own=True)
    for sub in first + second:
        start(X, sub, here, own=True)
    for sub in second + first:
        start(Y, sub, here, own=True)
    for swap in swaps:
        swap.start()
    owns = [
        pltpu.make_async_copy(mine, whole.at[(tp + fs) % 2, rep], own_sem.at[index])
        for index, (mine, whole) in enumerate(((x_ref, gx), (c_ref, gc)))
    ]
    for own in owns:
        own.start()

    def planes(step):
        if step == 0:
            return [(z, True, None, None)]
        return [
            (jnp.maximum(z - step, 0), z - step >= 0, UP, z < depth - 1),
            (jnp.minimum(z + step, depth - 1), z + step < depth, DOWN, z > 0),
        ]

    def both(one, other):
        return other if one is True else jnp.logical_and(one, other)

    def from_z(step):
        for at_z, there, way, more in planes(step):
            at = (at_z, y, tp)
            for sub in subs:
                arrive(sub, at, there)
                if step < depth - 1:
                    start(way, sub, at, both(there, more))
            for sub in first + second:
                start(X, sub, at, there)
            for sub in second + first:
                start(Y, sub, at, there)

    def cross(step):
        for at_z, there, _, _ in planes(step):
            for one, two in zip(first, second):
                across_x, across_y = (at_z, y, 1 - tp), (at_z, 1 - y, tp)
                arrive(one, across_x, there)
                start(Y, one, across_x, there)
                arrive(two, across_y, there)
                start(X, two, across_y, there)

    def rest(step):
        for at_z, there, _, _ in planes(step):
            for one, two in zip(first, second):
                arrive(one, (at_z, 1 - y, tp), there)
                arrive(two, (at_z, y, 1 - tp), there)
            for sub in subs:
                arrive(sub, (at_z, 1 - y, 1 - tp), there)

    cross(0)
    for step in range(1, depth):
        from_z(step)
        if step >= 2:
            cross(step - 1)
    if depth > 1:
        cross(depth - 1)
    for step in range(depth):
        rest(step)
    for own in owns:
        own.wait()
    for swap in swaps:
        swap.wait()
    for way, sub, at, condition, own in started:
        when(condition, lambda: copy(way, sub, at, own).wait_send())


def gather_all(reps, inputs, cotangent, w_up, w_down):
    rows, cols = inputs.shape
    whole = jax.ShapeDtypeStruct((2, reps, rows, cols), inputs.dtype)
    anywhere, vmem = pl.BlockSpec(memory_space=pl.ANY), pl.BlockSpec(memory_space=pltpu.VMEM)
    return pl.pallas_call(
        functools.partial(gather_kernel, reps),
        out_shape=(
            whole, whole,
            jax.ShapeDtypeStruct(w_up.shape, w_up.dtype), jax.ShapeDtypeStruct(w_down.shape, w_down.dtype),
        ),
        in_specs=[vmem, vmem, anywhere, anywhere],
        out_specs=[anywhere] * 4,
        scratch_shapes=[
            pltpu.SemaphoreType.DMA((4, 4, reps * 2)),
            pltpu.SemaphoreType.DMA((4, reps * 2)),
            pltpu.SemaphoreType.DMA((2, 2)),
            pltpu.SemaphoreType.DMA((2,)),
        ],
        compiler_params=pltpu.CompilerParams(collective_id=0, has_side_effects=True),
    )(inputs, cotangent, w_up, w_down)


def swapped(value, axis):
    return lax.ppermute(value, axis, [(0, 1), (1, 0)])


def few_tokens(reps, inputs, cotangent, w_up, w_down):
    rows = inputs.shape[0]
    rep, fs, tp = lax.axis_index("rep"), lax.axis_index("fs"), lax.axis_index("tp")
    gx, gc, up_other, down_other = gather_all(reps, inputs, cotangent, w_up, w_down)
    gx, gc = (value.reshape(2, -1, value.shape[-1]) for value in (gx, gc))
    preact = (
        jnp.dot(gx[0], w_up, preferred_element_type=jnp.float32)
        + jnp.dot(gx[1], up_other, preferred_element_type=jnp.float32)
    )
    act_grad = contract_cols(gc[0], w_down) + contract_cols(gc[1], down_other)
    relu_pre = jnp.maximum(preact, 0.0)
    squared = (relu_pre * relu_pre).astype(jnp.bfloat16)
    pre_grad = (2.0 * relu_pre * act_grad).astype(jnp.bfloat16)

    own_rows = lax.dynamic_slice_in_dim(pre_grad, rep * rows, rows, 0)
    part_own = contract_cols(own_rows, w_up).astype(jnp.bfloat16)
    part_other = contract_cols(own_rows, up_other).astype(jnp.bfloat16)
    same = fs == tp
    mine = jnp.where(same, part_own, part_other)
    theirs = swapped(jnp.where(same, part_other, part_own), "tp")

    up_theirs = swapped(contract_rows(gx[1], pre_grad).astype(jnp.bfloat16), "fs")
    down_theirs = swapped(contract_rows(squared, gc[1]).astype(jnp.bfloat16), "fs")
    grad_up = contract_rows(gx[0], pre_grad) + up_theirs.astype(jnp.float32)
    grad_down = contract_rows(squared, gc[0]) + down_theirs.astype(jnp.float32)
    grad_inputs = (mine.astype(jnp.float32) + theirs.astype(jnp.float32)).astype(jnp.bfloat16)
    return grad_inputs, grad_up, grad_down


def many_tokens(inputs, cotangent, w_up, w_down):
    rows_in, rows_cot = (
        lax.all_gather(inputs, "tp", axis=1, tiled=True),
        lax.all_gather(cotangent, "tp", axis=1, tiled=True),
    )
    cols_in, cols_cot = (
        lax.all_to_all(rows_in, "fs", split_axis=1, concat_axis=0, tiled=True),
        lax.all_to_all(rows_cot, "fs", split_axis=1, concat_axis=0, tiled=True),
    )
    full_up, full_down = (
        lax.all_gather(w_up, "fs", axis=0, tiled=True),
        lax.all_gather(w_down, "fs", axis=1, tiled=True),
    )
    act_grad = contract_cols(rows_cot, full_down)
    preact = jnp.dot(rows_in, full_up, preferred_element_type=jnp.float32)
    relu_pre = jnp.maximum(preact, 0.0)
    squared = (relu_pre * relu_pre).astype(jnp.bfloat16)
    pre_grad = (2.0 * relu_pre * act_grad).astype(jnp.bfloat16)
    partial_value = contract_cols(pre_grad, full_up)
    grad_inputs = lax.psum_scatter(
        partial_value.astype(jnp.bfloat16), "tp", scatter_dimension=1, tiled=True
    )
    grad_piece = lax.all_gather(pre_grad, "fs", axis=0, tiled=True)
    square_piece = lax.all_gather(squared, "fs", axis=0, tiled=True)
    local_up = contract_rows(cols_in, grad_piece)
    local_down = contract_rows(square_piece, cols_cot)
    slice_up = lax.psum_scatter(local_up, "rep", scatter_dimension=0, tiled=True)
    slice_down = lax.psum_scatter(local_down, "rep", scatter_dimension=0, tiled=True)
    grad_up = lax.all_gather(slice_up, "rep", axis=0, tiled=True)
    grad_down = lax.all_gather(slice_down, "rep", axis=0, tiled=True)
    return (grad_inputs, grad_up, grad_down)


def solution(mesh):
    reps, n_fs, n_tp = mesh.shape["rep"], mesh.shape["fs"], mesh.shape["tp"]

    def shards(inputs, cotangent, w_up, w_down):
        gathered = 2 * reps * n_tp * inputs.size * inputs.dtype.itemsize
        gradients = (w_up.size + w_down.size) * 4
        fits = n_fs == 2 and n_tp == 2 and reps % PAIR == 0 and inputs.shape[0] % 32 == 0
        if fits and gathered <= gradients:
            return few_tokens(reps, inputs, cotangent, w_up, w_down)
        return many_tokens(inputs, cotangent, w_up, w_down)

    return jax.shard_map(
        shards,
        mesh=mesh,
        in_specs=(P(("rep", "fs"), "tp"), P(("rep", "fs"), "tp"), P("fs", "tp"), P("tp", "fs")),
        out_specs=(P(("rep", "fs"), "tp"), P("fs", "tp"), P("tp", "fs")),
        check_vma=False,
    )
```

```python
import functools

import jax
import jax.numpy as jnp
from jax import lax
from jax.experimental import pallas as pl
from jax.experimental.pallas import tpu as pltpu
from jax.sharding import PartitionSpec as P

MESH = pl.DeviceIdType.MESH
X, Y, UP, DOWN = range(4)
PAIR = 2


def contract_rows(left, right):
    return lax.dot_general(
        left, right, (((0,), (0,)), ((), ())), preferred_element_type=jnp.float32
    )


def contract_cols(left, right):
    return lax.dot_general(
        left, right, (((1,), (1,)), ((), ())), preferred_element_type=jnp.float32
    )


def nearest(z, depth, index):
    near = jnp.minimum(z, depth - 1 - z)
    away = (index + 1) // 2
    around = z - away if index % 2 else z + away
    outward = jnp.where(z < depth - 1 - z, z + (index - near), z - (index - near))
    return jnp.where(index <= 2 * near, around, outward)


def hidden_kernel(reps, x_ref, c_ref, up_ref, down_ref,
                  pg_out, sq_out, x_out, c_out, mine_out, theirs_out,
                  gx, gc, up, down, pg, sq,
                  send_sem, recv_sem, swap_sem, own_sem, pair_send, pair_recv, out_sem):
    rep, fs, tp = lax.axis_index("rep"), lax.axis_index("fs"), lax.axis_index("tp")
    z, y = rep // PAIR, rep % PAIR
    depth = reps // PAIR
    height = x_ref.shape[0]
    half = height // 2
    plane = PAIR * height
    hidden = up.shape[2]
    target = {
        X: {"tp": 1 - tp},
        Y: {"rep": z * PAIR + (1 - y)},
        UP: {"rep": jnp.minimum(z + 1, depth - 1) * PAIR + y},
        DOWN: {"rep": jnp.maximum(z - 1, 0) * PAIR + y},
    }
    sibling = {"fs": 1 - fs}

    def when(condition, body):
        if condition is True:
            body()
        else:
            pl.when(condition)(body)

    barrier = pltpu.get_barrier_semaphore()

    def greet(device):
        pl.semaphore_signal(barrier, inc=1, device_id=device, device_id_type=MESH)

    greet(target[X])
    greet(target[Y])
    greet(sibling)
    when(z < depth - 1, lambda: greet(target[UP]))
    when(z > 0, lambda: greet(target[DOWN]))
    pl.semaphore_wait(barrier, 3 + (z < depth - 1).astype(jnp.int32) + (z > 0).astype(jnp.int32))

    def token(core, source, extra=0):
        return pl.multiple_of((core * reps + source) * height + extra, half)

    def copy(way, sub, at, own=False):
        at_z, at_y, at_t = at
        array, part = sub
        source = at_z * PAIR + at_y
        there = (gx, gc)[array].at[(at_t + fs) % 2, pl.ds(token(fs, source, part * half), half)]
        here = (x_ref, c_ref)[array].at[pl.ds(part * half, half)] if own else there
        index, piece = array * 2 + part, source * 2 + at_t
        return pltpu.make_async_remote_copy(
            src_ref=here, dst_ref=there,
            send_sem=send_sem.at[way, index, piece],
            recv_sem=recv_sem.at[index, piece],
            device_id=target[way], device_id_type=MESH,
        )

    started, locals_started = [], []

    def start(way, sub, at, condition=True, own=False):
        when(condition, lambda: copy(way, sub, at, own).start())
        started.append((way, sub, at, condition, own))

    def arrive(sub, at):
        copy(X, sub, at).wait_recv()

    def put(here, there, sem):
        moved = pltpu.make_async_copy(here, there, sem)
        moved.start()
        locals_started.append(moved)
        return moved

    subs = [(array, part) for part in range(2) for array in range(2)]
    first = [(array, 0) for array in range(2)]
    second = [(array, 1) for array in range(2)]
    planes = [nearest(z, depth, index) for index in range(depth)]

    here = (z, y, tp)
    for sub in subs:
        start(UP, sub, here, z < depth - 1, own=True)
        start(DOWN, sub, here, z > 0, own=True)
    for sub in first + second:
        start(X, sub, here, own=True)
    for sub in second + first:
        start(Y, sub, here, own=True)
    own_slot = (tp + fs) % 2
    own_rows = pl.ds(token(fs, rep), height)
    owns = [
        pltpu.make_async_copy(from_ref, into, own_sem.at[index])
        for index, (from_ref, into) in enumerate((
            (x_ref, gx.at[own_slot, own_rows]), (c_ref, gc.at[own_slot, own_rows]),
            (up_ref, up.at[0]), (down_ref, down.at[0]),
        ))
    ]
    for own in owns:
        own.start()
    swaps = [
        pltpu.make_async_remote_copy(
            src_ref=from_ref, dst_ref=into.at[1], send_sem=swap_sem.at[0, index], recv_sem=swap_sem.at[1, index],
            device_id=sibling, device_id_type=MESH,
        )
        for index, (from_ref, into) in enumerate(((up_ref, up), (down_ref, down)))
    ]
    for swap in swaps:
        swap.start()

    def from_z(index):
        at_z = planes[index]
        at = (at_z, y, tp)
        for sub in subs:
            arrive(sub, at)
            start(UP, sub, at, jnp.logical_and(at_z < z, z < depth - 1))
            start(DOWN, sub, at, jnp.logical_and(at_z > z, z > 0))
        for sub in first + second:
            start(X, sub, at)
        for sub in second + first:
            start(Y, sub, at)

    def cross(index):
        at_z = planes[index]
        for one, two in zip(first, second):
            across_x, across_y = (at_z, y, 1 - tp), (at_z, 1 - y, tp)
            arrive(one, across_x)
            start(Y, one, across_x)
            arrive(two, across_y)
            start(X, two, across_y)

    def pair_copy(index, array, slot, core):
        rows = pl.ds(token(core, planes[index] * PAIR), plane)
        held = (gx, gc)[array]
        return pltpu.make_async_remote_copy(
            src_ref=held.at[slot, rows], dst_ref=held.at[1 - slot, rows],
            send_sem=pair_send.at[array * 2 + slot, index], recv_sem=pair_recv.at[array * 2 + slot, index],
            device_id=sibling, device_id_type=MESH,
        )

    quads = [(array, slot) for array in range(2) for slot in range(2)]

    def keep(index, core, number):
        rows = pl.ds(token(core, planes[index] * PAIR), plane)
        put(gx.at[0, rows], x_out.at[rows], out_sem.at[0, number, index])
        put(gc.at[0, rows], c_out.at[rows], out_sem.at[1, number, index])

    def rest(index):
        at_z = planes[index]
        for one, two in zip(first, second):
            arrive(one, (at_z, 1 - y, tp))
            arrive(two, (at_z, y, 1 - tp))
        for sub in subs:
            arrive(sub, (at_z, 1 - y, 1 - tp))
        for array, slot in quads:
            pair_copy(index, array, slot, fs).start()
        keep(index, fs, 0)

    def compute(index, core, number):
        rows = pl.ds(token(core, planes[index] * PAIR), plane)
        tile = hidden // 4

        @pl.loop(0, hidden // tile)
        def _(step):
            cols = pl.ds(pl.multiple_of(step * tile, tile), tile)
            preact = (
                jnp.dot(gx[0, rows, :], up[0, :, cols], preferred_element_type=jnp.float32)
                + jnp.dot(gx[1, rows, :], up[1, :, cols], preferred_element_type=jnp.float32)
            )
            act_grad = contract_cols(gc[0, rows, :], down[0, cols, :]) + contract_cols(gc[1, rows, :], down[1, cols, :])
            relu_pre = jnp.maximum(preact, 0.0)
            sq[rows, cols] = (relu_pre * relu_pre).astype(sq.dtype)
            pg[rows, cols] = (2.0 * relu_pre * act_grad).astype(pg.dtype)

        put(pg.at[rows], pg_out.at[rows], out_sem.at[2, number, index])
        put(sq.at[rows], sq_out.at[rows], out_sem.at[3, number, index])

    def compute_other(index):
        for array, slot in quads:
            pair_copy(index, array, slot, 1 - fs).wait_recv()
        keep(index, 1 - fs, 1)
        compute(index, 1 - fs, 1)

    def partial():
        width = mine_out.shape[1]
        tile = width // 4

        @pl.loop(0, width // tile)
        def _(step):
            cols = pl.ds(pl.multiple_of(step * tile, tile), tile)
            for slot, into in ((own_slot, mine_out), (1 - own_slot, theirs_out)):
                into[:, cols] = contract_cols(pg[own_rows, :], up[slot, cols, :]).astype(into.dtype)

    cross(0)
    for index in range(1, min(3, depth)):
        from_z(index)
    for own in owns:
        own.wait()
    rest(0)
    for swap in swaps:
        swap.wait()
    compute(0, fs, 0)
    for index in range(3, depth):
        from_z(index)
    if depth > 1:
        cross(1)
    compute_other(0)
    for index in range(2, depth):
        cross(index)
        rest(index - 1)
        compute(index - 1, fs, 0)
        if index == 2:
            partial()
        compute_other(index - 1)
    if depth <= 2:
        partial()
    if depth > 1:
        rest(depth - 1)
        compute(depth - 1, fs, 0)
        compute_other(depth - 1)
    for way, sub, at, condition, own in started:
        when(condition, lambda: copy(way, sub, at, own).wait_send())
    for index in range(depth):
        for array, slot in quads:
            pair_copy(index, array, slot, fs).wait_send()
    for moved in locals_started:
        moved.wait()


def hidden_gradients(reps, inputs, cotangent, w_up, w_down):
    rows, cols = inputs.shape
    hidden = w_up.shape[1]
    tokens, depth = 2 * reps * rows, reps // PAIR
    low = inputs.dtype
    anywhere, vmem = pl.BlockSpec(memory_space=pl.ANY), pl.BlockSpec(memory_space=pltpu.VMEM)
    whole, wide, part = (tokens, cols), (tokens, hidden), (rows, cols)
    flops = 8 * tokens * cols * 2 * hidden
    return pl.pallas_call(
        functools.partial(hidden_kernel, reps),
        out_shape=[jax.ShapeDtypeStruct(shape, low) for shape in (wide, wide, whole, whole, part, part)],
        in_specs=[vmem, vmem, anywhere, anywhere],
        out_specs=[anywhere] * 4 + [vmem] * 2,
        scratch_shapes=[
            pltpu.VMEM((2,) + whole, low),
            pltpu.VMEM((2,) + whole, low),
            pltpu.VMEM((2,) + w_up.shape, low),
            pltpu.VMEM((2,) + w_down.shape, low),
            pltpu.VMEM(wide, low),
            pltpu.VMEM(wide, low),
            pltpu.SemaphoreType.DMA((4, 4, reps * 2)),
            pltpu.SemaphoreType.DMA((4, reps * 2)),
            pltpu.SemaphoreType.DMA((2, 2)),
            pltpu.SemaphoreType.DMA((4,)),
            pltpu.SemaphoreType.DMA((4, depth)),
            pltpu.SemaphoreType.DMA((4, depth)),
            pltpu.SemaphoreType.DMA((4, 2, depth)),
        ],
        cost_estimate=pl.CostEstimate(flops=flops, bytes_accessed=tokens * hidden * 8, transcendentals=0),
        compiler_params=pltpu.CompilerParams(
            collective_id=0, has_side_effects=True, vmem_limit_bytes=60 * 1024 * 1024
        ),
    )(inputs, cotangent, w_up, w_down)


def few_tokens(reps, inputs, cotangent, w_up, w_down):
    pre_grad, squared, cols_in, cols_cot, mine, theirs = hidden_gradients(reps, inputs, cotangent, w_up, w_down)
    theirs = lax.ppermute(theirs, "tp", [(0, 1), (1, 0)])
    grad_up = contract_rows(cols_in, pre_grad)
    grad_down = contract_rows(squared, cols_cot)
    grad_inputs = (mine.astype(jnp.float32) + theirs.astype(jnp.float32)).astype(jnp.bfloat16)
    return grad_inputs, grad_up, grad_down


def many_tokens(inputs, cotangent, w_up, w_down):
    rows_in, rows_cot = (
        lax.all_gather(inputs, "tp", axis=1, tiled=True),
        lax.all_gather(cotangent, "tp", axis=1, tiled=True),
    )
    cols_in, cols_cot = (
        lax.all_to_all(rows_in, "fs", split_axis=1, concat_axis=0, tiled=True),
        lax.all_to_all(rows_cot, "fs", split_axis=1, concat_axis=0, tiled=True),
    )
    full_up, full_down = (
        lax.all_gather(w_up, "fs", axis=0, tiled=True),
        lax.all_gather(w_down, "fs", axis=1, tiled=True),
    )
    act_grad = contract_cols(rows_cot, full_down)
    preact = jnp.dot(rows_in, full_up, preferred_element_type=jnp.float32)
    relu_pre = jnp.maximum(preact, 0.0)
    squared = (relu_pre * relu_pre).astype(jnp.bfloat16)
    pre_grad = (2.0 * relu_pre * act_grad).astype(jnp.bfloat16)
    partial_value = contract_cols(pre_grad, full_up)
    grad_inputs = lax.psum_scatter(
        partial_value.astype(jnp.bfloat16), "tp", scatter_dimension=1, tiled=True
    )
    grad_piece = lax.all_gather(pre_grad, "fs", axis=0, tiled=True)
    square_piece = lax.all_gather(squared, "fs", axis=0, tiled=True)
    local_up = contract_rows(cols_in, grad_piece)
    local_down = contract_rows(square_piece, cols_cot)
    slice_up = lax.psum_scatter(local_up, "rep", scatter_dimension=0, tiled=True)
    slice_down = lax.psum_scatter(local_down, "rep", scatter_dimension=0, tiled=True)
    grad_up = lax.all_gather(slice_up, "rep", axis=0, tiled=True)
    grad_down = lax.all_gather(slice_down, "rep", axis=0, tiled=True)
    return (grad_inputs, grad_up, grad_down)


def solution(mesh):
    reps, n_fs, n_tp = mesh.shape["rep"], mesh.shape["fs"], mesh.shape["tp"]

    def shards(inputs, cotangent, w_up, w_down):
        gathered = 2 * reps * n_tp * inputs.size * inputs.dtype.itemsize
        gradients = (w_up.size + w_down.size) * 4
        fits = n_fs == 2 and n_tp == 2 and reps % PAIR == 0 and inputs.shape[0] % 32 == 0
        if fits and gathered <= gradients:
            return few_tokens(reps, inputs, cotangent, w_up, w_down)
        return many_tokens(inputs, cotangent, w_up, w_down)

    return jax.shard_map(
        shards,
        mesh=mesh,
        in_specs=(P(("rep", "fs"), "tp"), P(("rep", "fs"), "tp"), P("fs", "tp"), P("tp", "fs")),
        out_specs=(P(("rep", "fs"), "tp"), P("fs", "tp"), P("tp", "fs")),
        check_vma=False,
    )
```

```python
import functools

import jax
import jax.numpy as jnp
from jax import lax
from jax.experimental import pallas as pl
from jax.experimental.pallas import tpu as pltpu
from jax.sharding import PartitionSpec as P

MESH = pl.DeviceIdType.MESH
X, Y, UP, DOWN = range(4)
PAIR = 2


def contract_rows(left, right):
    return lax.dot_general(
        left, right, (((0,), (0,)), ((), ())), preferred_element_type=jnp.float32
    )


def contract_cols(left, right):
    return lax.dot_general(
        left, right, (((1,), (1,)), ((), ())), preferred_element_type=jnp.float32
    )


def nearest(z, depth, index):
    near = jnp.minimum(z, depth - 1 - z)
    away = (index + 1) // 2
    around = z - away if index % 2 else z + away
    outward = jnp.where(z < depth - 1 - z, z + (index - near), z - (index - near))
    return jnp.where(index <= 2 * near, around, outward)


def hidden_kernel(reps, x_ref, c_ref, up_ref, down_ref,
                  pg_out, sq_out, x_out, c_out, mine_out, theirs_out,
                  gx, gc, up, down, pg, sq,
                  send_sem, recv_sem, swap_sem, own_sem, pair_send, pair_recv, out_sem):
    rep, fs, tp = lax.axis_index("rep"), lax.axis_index("fs"), lax.axis_index("tp")
    z, y = rep // PAIR, rep % PAIR
    depth = reps // PAIR
    height = x_ref.shape[0]
    half = height // 2
    plane = PAIR * height
    hidden = up.shape[2]
    target = {
        X: {"tp": 1 - tp},
        Y: {"rep": z * PAIR + (1 - y)},
        UP: {"rep": jnp.minimum(z + 1, depth - 1) * PAIR + y},
        DOWN: {"rep": jnp.maximum(z - 1, 0) * PAIR + y},
    }
    sibling = {"fs": 1 - fs}

    def when(condition, body):
        if condition is True:
            body()
        else:
            pl.when(condition)(body)

    barrier = pltpu.get_barrier_semaphore()

    def greet(device):
        pl.semaphore_signal(barrier, inc=1, device_id=device, device_id_type=MESH)

    greet(target[X])
    greet(target[Y])
    greet(sibling)
    when(z < depth - 1, lambda: greet(target[UP]))
    when(z > 0, lambda: greet(target[DOWN]))
    pl.semaphore_wait(barrier, 3 + (z < depth - 1).astype(jnp.int32) + (z > 0).astype(jnp.int32))

    def token(core, source, extra=0):
        return pl.multiple_of((core * reps + source) * height + extra, half)

    def copy(way, sub, at, own=False):
        at_z, at_y, at_t = at
        array, part = sub
        source = at_z * PAIR + at_y
        there = (gx, gc)[array].at[(at_t + fs) % 2, pl.ds(token(fs, source, part * half), half)]
        here = (x_ref, c_ref)[array].at[pl.ds(part * half, half)] if own else there
        index, piece = array * 2 + part, source * 2 + at_t
        return pltpu.make_async_remote_copy(
            src_ref=here, dst_ref=there,
            send_sem=send_sem.at[way, index, piece],
            recv_sem=recv_sem.at[index, piece],
            device_id=target[way], device_id_type=MESH,
        )

    started, locals_started = [], []

    def start(way, sub, at, condition=True, own=False):
        when(condition, lambda: copy(way, sub, at, own).start())
        started.append((way, sub, at, condition, own))

    def arrive(sub, at):
        copy(X, sub, at).wait_recv()

    def put(here, there, sem):
        moved = pltpu.make_async_copy(here, there, sem)
        moved.start()
        locals_started.append(moved)
        return moved

    subs = [(array, part) for part in range(2) for array in range(2)]
    first = [(array, 0) for array in range(2)]
    second = [(array, 1) for array in range(2)]
    planes = [nearest(z, depth, index) for index in range(depth)]

    here = (z, y, tp)
    for sub in subs:
        start(UP, sub, here, z < depth - 1, own=True)
        start(DOWN, sub, here, z > 0, own=True)
    for sub in first + second:
        start(X, sub, here, own=True)
    for sub in second + first:
        start(Y, sub, here, own=True)
    own_slot = (tp + fs) % 2
    own_rows = pl.ds(token(fs, rep), height)
    owns = [
        pltpu.make_async_copy(from_ref, into, own_sem.at[index])
        for index, (from_ref, into) in enumerate((
            (x_ref, gx.at[own_slot, own_rows]), (c_ref, gc.at[own_slot, own_rows]),
            (up_ref, up.at[0]), (down_ref, down.at[0]),
        ))
    ]
    for own in owns:
        own.start()
    swaps = [
        pltpu.make_async_remote_copy(
            src_ref=from_ref, dst_ref=into.at[1], send_sem=swap_sem.at[0, index], recv_sem=swap_sem.at[1, index],
            device_id=sibling, device_id_type=MESH,
        )
        for index, (from_ref, into) in enumerate(((up_ref, up), (down_ref, down)))
    ]
    for swap in swaps:
        swap.start()

    def from_z(index):
        at_z = planes[index]
        at = (at_z, y, tp)
        for sub in subs:
            arrive(sub, at)
            start(UP, sub, at, jnp.logical_and(at_z < z, z < depth - 1))
            start(DOWN, sub, at, jnp.logical_and(at_z > z, z > 0))
        for sub in first + second:
            start(X, sub, at)
        for sub in second + first:
            start(Y, sub, at)

    def cross(index):
        at_z = planes[index]
        for one, two in zip(first, second):
            across_x, across_y = (at_z, y, 1 - tp), (at_z, 1 - y, tp)
            arrive(one, across_x)
            start(Y, one, across_x)
            arrive(two, across_y)
            start(X, two, across_y)

    def pair_copy(index, array, slot, core):
        rows = pl.ds(token(core, planes[index] * PAIR), plane)
        held = (gx, gc)[array]
        return pltpu.make_async_remote_copy(
            src_ref=held.at[slot, rows], dst_ref=held.at[1 - slot, rows],
            send_sem=pair_send.at[array * 2 + slot, index], recv_sem=pair_recv.at[array * 2 + slot, index],
            device_id=sibling, device_id_type=MESH,
        )

    quads = [(array, slot) for array in range(2) for slot in range(2)]

    def keep(index, core, number):
        rows = pl.ds(token(core, planes[index] * PAIR), plane)
        put(gx.at[0, rows], x_out.at[rows], out_sem.at[0, number, index])
        put(gc.at[0, rows], c_out.at[rows], out_sem.at[1, number, index])

    def rest(index):
        at_z = planes[index]
        for one, two in zip(first, second):
            arrive(one, (at_z, 1 - y, tp))
            arrive(two, (at_z, y, 1 - tp))
        for sub in subs:
            arrive(sub, (at_z, 1 - y, 1 - tp))
        for array, slot in quads:
            pair_copy(index, array, slot, fs).start()
        keep(index, fs, 0)

    def compute(index, core, number):
        rows = pl.ds(token(core, planes[index] * PAIR), plane)
        tile = hidden // 4

        @pl.loop(0, hidden // tile)
        def _(step):
            cols = pl.ds(pl.multiple_of(step * tile, tile), tile)
            preact = (
                jnp.dot(gx[0, rows, :], up[0, :, cols], preferred_element_type=jnp.float32)
                + jnp.dot(gx[1, rows, :], up[1, :, cols], preferred_element_type=jnp.float32)
            )
            act_grad = contract_cols(gc[0, rows, :], down[0, cols, :]) + contract_cols(gc[1, rows, :], down[1, cols, :])
            relu_pre = jnp.maximum(preact, 0.0)
            sq[rows, cols] = (relu_pre * relu_pre).astype(sq.dtype)
            pg[rows, cols] = (2.0 * relu_pre * act_grad).astype(pg.dtype)

        put(pg.at[rows], pg_out.at[rows], out_sem.at[2, number, index])
        put(sq.at[rows], sq_out.at[rows], out_sem.at[3, number, index])

    def compute_other(index):
        for array, slot in quads:
            pair_copy(index, array, slot, 1 - fs).wait_recv()
        keep(index, 1 - fs, 1)
        compute(index, 1 - fs, 1)

    def partial():
        width = mine_out.shape[1]
        tile = width // 4

        @pl.loop(0, width // tile)
        def _(step):
            cols = pl.ds(pl.multiple_of(step * tile, tile), tile)
            for slot, into in ((own_slot, mine_out), (1 - own_slot, theirs_out)):
                into[:, cols] = contract_cols(pg[own_rows, :], up[slot, cols, :]).astype(into.dtype)

    cross(0)
    for index in range(1, min(3, depth)):
        from_z(index)
    for own in owns:
        own.wait()
    rest(0)
    for swap in swaps:
        swap.wait()
    compute(0, fs, 0)
    for index in range(3, depth):
        from_z(index)
    if depth > 1:
        cross(1)
    compute_other(0)
    for index in range(2, depth):
        rest(index - 1)
        compute(index - 1, fs, 0)
        cross(index)
        if index == 2:
            partial()
        compute_other(index - 1)
    if depth <= 2:
        partial()
    if depth > 1:
        rest(depth - 1)
        compute(depth - 1, fs, 0)
        compute_other(depth - 1)
    for way, sub, at, condition, own in started:
        when(condition, lambda: copy(way, sub, at, own).wait_send())
    for index in range(depth):
        for array, slot in quads:
            pair_copy(index, array, slot, fs).wait_send()
    for moved in locals_started:
        moved.wait()


def hidden_gradients(reps, inputs, cotangent, w_up, w_down):
    rows, cols = inputs.shape
    hidden = w_up.shape[1]
    tokens, depth = 2 * reps * rows, reps // PAIR
    low = inputs.dtype
    anywhere, vmem = pl.BlockSpec(memory_space=pl.ANY), pl.BlockSpec(memory_space=pltpu.VMEM)
    whole, wide, part = (tokens, cols), (tokens, hidden), (rows, cols)
    flops = 8 * tokens * cols * 2 * hidden
    return pl.pallas_call(
        functools.partial(hidden_kernel, reps),
        out_shape=[jax.ShapeDtypeStruct(shape, low) for shape in (wide, wide, whole, whole, part, part)],
        in_specs=[vmem, vmem, anywhere, anywhere],
        out_specs=[anywhere] * 4 + [vmem] * 2,
        scratch_shapes=[
            pltpu.VMEM((2,) + whole, low),
            pltpu.VMEM((2,) + whole, low),
            pltpu.VMEM((2,) + w_up.shape, low),
            pltpu.VMEM((2,) + w_down.shape, low),
            pltpu.VMEM(wide, low),
            pltpu.VMEM(wide, low),
            pltpu.SemaphoreType.DMA((4, 4, reps * 2)),
            pltpu.SemaphoreType.DMA((4, reps * 2)),
            pltpu.SemaphoreType.DMA((2, 2)),
            pltpu.SemaphoreType.DMA((4,)),
            pltpu.SemaphoreType.DMA((4, depth)),
            pltpu.SemaphoreType.DMA((4, depth)),
            pltpu.SemaphoreType.DMA((4, 2, depth)),
        ],
        cost_estimate=pl.CostEstimate(flops=flops, bytes_accessed=tokens * hidden * 8, transcendentals=0),
        compiler_params=pltpu.CompilerParams(
            collective_id=0, has_side_effects=True, vmem_limit_bytes=60 * 1024 * 1024
        ),
    )(inputs, cotangent, w_up, w_down)


def few_tokens(reps, inputs, cotangent, w_up, w_down):
    pre_grad, squared, cols_in, cols_cot, mine, theirs = hidden_gradients(reps, inputs, cotangent, w_up, w_down)
    theirs = lax.ppermute(theirs, "tp", [(0, 1), (1, 0)])
    grad_up = contract_rows(cols_in, pre_grad)
    grad_down = contract_rows(squared, cols_cot)
    grad_inputs = (mine.astype(jnp.float32) + theirs.astype(jnp.float32)).astype(jnp.bfloat16)
    return grad_inputs, grad_up, grad_down


def many_tokens(inputs, cotangent, w_up, w_down):
    rows_in, rows_cot = (
        lax.all_gather(inputs, "tp", axis=1, tiled=True),
        lax.all_gather(cotangent, "tp", axis=1, tiled=True),
    )
    cols_in, cols_cot = (
        lax.all_to_all(rows_in, "fs", split_axis=1, concat_axis=0, tiled=True),
        lax.all_to_all(rows_cot, "fs", split_axis=1, concat_axis=0, tiled=True),
    )
    full_up, full_down = (
        lax.all_gather(w_up, "fs", axis=0, tiled=True),
        lax.all_gather(w_down, "fs", axis=1, tiled=True),
    )
    act_grad = contract_cols(rows_cot, full_down)
    preact = jnp.dot(rows_in, full_up, preferred_element_type=jnp.float32)
    relu_pre = jnp.maximum(preact, 0.0)
    squared = (relu_pre * relu_pre).astype(jnp.bfloat16)
    pre_grad = (2.0 * relu_pre * act_grad).astype(jnp.bfloat16)
    partial_value = contract_cols(pre_grad, full_up)
    grad_inputs = lax.psum_scatter(
        partial_value.astype(jnp.bfloat16), "tp", scatter_dimension=1, tiled=True
    )
    grad_piece = lax.all_gather(pre_grad, "fs", axis=0, tiled=True)
    square_piece = lax.all_gather(squared, "fs", axis=0, tiled=True)
    local_up = contract_rows(cols_in, grad_piece)
    local_down = contract_rows(square_piece, cols_cot)
    slice_up = lax.psum_scatter(local_up, "rep", scatter_dimension=0, tiled=True)
    slice_down = lax.psum_scatter(local_down, "rep", scatter_dimension=0, tiled=True)
    grad_up = lax.all_gather(slice_up, "rep", axis=0, tiled=True)
    grad_down = lax.all_gather(slice_down, "rep", axis=0, tiled=True)
    return (grad_inputs, grad_up, grad_down)


def solution(mesh):
    reps, n_fs, n_tp = mesh.shape["rep"], mesh.shape["fs"], mesh.shape["tp"]

    def shards(inputs, cotangent, w_up, w_down):
        gathered = 2 * reps * n_tp * inputs.size * inputs.dtype.itemsize
        gradients = (w_up.size + w_down.size) * 4
        fits = n_fs == 2 and n_tp == 2 and reps % PAIR == 0 and inputs.shape[0] % 32 == 0
        if fits and gathered <= gradients:
            return few_tokens(reps, inputs, cotangent, w_up, w_down)
        return many_tokens(inputs, cotangent, w_up, w_down)

    return jax.shard_map(
        shards,
        mesh=mesh,
        in_specs=(P(("rep", "fs"), "tp"), P(("rep", "fs"), "tp"), P("fs", "tp"), P("tp", "fs")),
        out_specs=(P(("rep", "fs"), "tp"), P("fs", "tp"), P("tp", "fs")),
        check_vma=False,
    )
```
